32 devices in a mesh: sp: 16 (over z, y, core), tp: 2 (over x).
Axes of the slice: x: 2, y: 2, z: 4, core: 2. Of those that a mesh axis runs over, the one named last changes fastest.
Arguments:
- tokens: bfloat16 [1024, 4, 2048], P(('sp', 'tp')), may hold values from -16 to 16
- norm_gain: float32 [2048], replicated, may hold values from 0.1 to 1.9
- w_query: bfloat16 [2048, 2048], P('sp', 'tp'), may hold values from -0.125 to 0.125
- w_forget: bfloat16 [2048, 2048], P('sp', 'tp'), may hold values from -0.125 to 0.125
- w_value: bfloat16 [2048, 2048], P('sp', 'tp'), may hold values from -0.125 to 0.125
- floor_gap: float32 [2048], P('tp'), may hold values from 0 to 0.15, as said below
- head_gain: float32 [2048], P('tp'), may hold values from 0.1 to 1.9
- w_out: bfloat16 [2048, 2048], P('tp', 'sp'), may hold values from -0.125 to 0.125
Outputs:
- mixed: bfloat16 [1024, 4, 2048], P(('sp', 'tp'))
The draws below stay inside these ranges and needn't reach their ends.
Inputs may be any that keep to these rules, and one draw needn't show every extreme that they name: `floor_gap`: positive, at least 0.5 / 1024 and at most 0.15.
All inputs are finite; a program needn't handle non-finite values.
Results may differ from the reference program's by a relative error of at most 0.014.
Values may be sent and summed in bfloat16 or wider, within the bound.
A program may use at most 128 MiB of HBM per device.

```python
import math
import jax
import jax.numpy as jnp
from jax import lax

D = 2048
HEADS = 16
KEY_DIM = 128
VAL_DIM = 128
SEQS = 4
HK = 2048
HV = 2048
LENGTH = 1024
N_TP = 2


def draw_tokens(key, part):
    noise_key, scale_key, aim_key, level_key = jax.random.split(key, 4)
    direction = jnp.clip(jax.random.normal(aim_key, (D,), jnp.float32), -4.0, 4.0)
    levels = jax.random.uniform(level_key, (LENGTH // 128 + 1, SEQS), jnp.float32, -2.5, 2.5)
    block_index = jnp.arange(LENGTH) // 128
    shift = levels[block_index][:, :, None] * direction
    base = jnp.clip(jax.random.normal(noise_key, (LENGTH, SEQS, D), jnp.float32), -6.0, 6.0)
    return (base + shift).astype(jnp.bfloat16)


def draw_floor_gap(key, part):
    kind_key, fast_key, slow_key = jax.random.split(jax.random.fold_in(key, 7), 3)
    slow_head = jax.random.randint(kind_key, (HEADS, 1), 0, 2) > 0
    fast_gap = jnp.exp(jax.random.uniform(fast_key, (HEADS, KEY_DIM), jnp.float32, math.log(0.04), math.log(0.145)))
    slow_gap = jnp.exp(jax.random.uniform(slow_key, (HEADS, KEY_DIM), jnp.float32, math.log(0.5), math.log(3.0))) / LENGTH
    return jnp.where(slow_head, slow_gap, fast_gap).reshape(HEADS * KEY_DIM).astype(jnp.float32)


def block_scale(own_key, extent, shards, low, largest):
    def one(position, blocks):
        draws = jax.random.uniform(jax.random.fold_in(jax.random.fold_in(own_key, 6), position), (blocks,), jnp.float32, low / len(shards), largest / len(shards))
        return jnp.repeat(jnp.exp(draws), extent[position] // blocks).reshape((-1,) + (1,) * (len(extent) - position - 1))

    level = one(*shards[0])
    for cut in shards[1:]:
        level = level * one(*cut)
    return level


def gaussian(key, shape, scale, reach, pieces=(), kind=jnp.bfloat16):
    result = jax.random.normal(key, shape, jnp.float32) * scale
    if len(pieces) > 0:
        result = block_scale(key, shape, pieces, -0.22, 0.18) * result
    return jnp.clip(result, min=-reach, max=reach).astype(kind)


def setup_inputs(seed: int = 0) -> dict:
    keys = jax.random.split(jax.random.key(seed), 9)
    tokens = draw_tokens(jax.random.fold_in(keys[8], 71), 0)
    norm_gain = jnp.clip(1.0 + 0.18 * jax.random.normal(keys[1], (D,), jnp.float32), 0.1, 1.9)
    w_query = gaussian(keys[2], (D, HK), D ** -0.5, 0.125, ((0, 16), (1, 2)))
    w_forget = gaussian(keys[3], (D, HK), D ** -0.5, 0.125, ((0, 16), (1, 2)))
    w_value = gaussian(keys[4], (D, HV), D ** -0.5, 0.125, ((0, 16), (1, 2)))
    floor_gap = draw_floor_gap(jax.random.fold_in(keys[8], 71), 0)
    head_gain = jnp.clip(1.0 + 0.18 * jax.random.normal(keys[6], (HV,), jnp.float32), 0.1, 1.9)
    w_out = gaussian(keys[7], (HV, D), HV ** -0.5, 0.125, ((0, 2), (1, 16)))
    return dict(tokens=tokens, norm_gain=norm_gain, w_query=w_query, w_forget=w_forget, w_value=w_value, floor_gap=floor_gap, head_gain=head_gain, w_out=w_out)


eps_norm = 1e-06
highest = lax.Precision.HIGHEST

def stored(value):
    return lax.optimization_barrier(value.astype(jnp.bfloat16)).astype(jnp.float32)

def reference(tokens, norm_gain, w_query, w_forget, w_value, floor_gap, head_gain, w_out):
    length, sequences = (tokens.shape[0], tokens.shape[1])
    flat = tokens.astype(jnp.float32)
    scale = lax.rsqrt(lax.optimization_barrier(jnp.mean(flat * flat, axis=-1, keepdims=True)) + eps_norm)
    normed = (flat * scale * norm_gain).astype(jnp.bfloat16).reshape(length * sequences, D)
    query_pre = stored(jnp.dot(normed, w_query, preferred_element_type=jnp.float32))
    forget_pre = stored(jnp.dot(normed, w_forget, preferred_element_type=jnp.float32))
    value_pre = stored(jnp.dot(normed, w_value, preferred_element_type=jnp.float32))
    block_len = math.gcd(length, 64)
    block_count = length // block_len

    def blocks(value, channels):
        return value.reshape(block_count, block_len, sequences, HEADS, channels)
    query = jax.nn.silu(blocks(query_pre, KEY_DIM))
    inkey = floor_gap.reshape(HEADS, KEY_DIM) * jax.nn.sigmoid(-blocks(forget_pre, KEY_DIM))
    log_forget = jnp.log1p(-inkey)
    values = blocks(value_pre, VAL_DIM)
    causal = jnp.tril(jnp.ones((block_len, block_len), dtype=bool))

    def advance(state, inputs):
        query_block, key_block, value_block, forget_block = inputs
        cumulative = jnp.cumsum(forget_block, axis=0)
        spread = cumulative[:, None] - cumulative[None, :]
        decay = jnp.exp(jnp.where(causal[:, :, None, None, None], spread, -jnp.inf))
        scores = jnp.einsum('tshk,ushk,tushk->shtu', query_block, key_block, decay, precision=highest)
        inside = jnp.einsum('shtu,ushv->tshv', scores, value_block, precision=highest)
        carried = jnp.einsum('tshk,shkv->tshv', query_block * jnp.exp(cumulative), state, precision=highest)
        final = cumulative[-1]
        weighted = key_block * jnp.exp(final[None] - cumulative)
        new_state = jnp.exp(final)[..., None] * state + jnp.einsum('ushk,ushv->shkv', weighted, value_block, precision=highest)
        return (new_state, inside + carried)
    start_state = jnp.zeros((sequences, HEADS, KEY_DIM, VAL_DIM), jnp.float32)
    _, recurrent = lax.scan(advance, start_state, (query, inkey, values, log_forget))
    mean_square = lax.optimization_barrier(jnp.mean(recurrent * recurrent, axis=-1, keepdims=True))
    hidden = recurrent * lax.rsqrt(mean_square + eps_norm) * head_gain.reshape(HEADS, VAL_DIM)
    hidden = hidden.astype(jnp.bfloat16).reshape(length * sequences, HEADS * VAL_DIM)
    group_width = HEADS * VAL_DIM // N_TP
    total = jnp.zeros((length * sequences, D), jnp.float32)
    for group in range(N_TP):
        lower = group * group_width
        partial_value = jnp.dot(hidden[:, lower:lower + group_width], w_out[lower:lower + group_width], preferred_element_type=jnp.float32)
        total = total + lax.optimization_barrier(partial_value.astype(jnp.bfloat16)).astype(jnp.float32)
    return total.astype(jnp.bfloat16).reshape(length, sequences, D)
```

```python
import functools
import math

import jax
import jax.numpy as jnp
from jax import lax
from jax.experimental import pallas as pl
from jax.experimental.pallas import tpu as pltpu
from jax.sharding import PartitionSpec as P

KEY_DIM = 128
VAL_DIM = 128
eps_norm = 1e-06
MESH = pl.DeviceIdType.MESH
f32 = jnp.float32
bf16 = jnp.bfloat16


def nt(a, b):
    return lax.dot_general(a, b, (((1,), (1,)), ((), ())), preferred_element_type=f32)


def tn(a, b):
    return lax.dot_general(a, b, (((0,), (0,)), ((), ())), preferred_element_type=f32)


def kernel(
    dims,
    tok, gain, wq, wf, wv, wo, gap, hgain,
    out,
    X, N, W, PJ, IK, CUM, QS, INS, U, DEC, SS, DS, SR, DR, ACC, HB, OB, PB, RSB, RB,
    w_send, w_recv, t_send, t_recv, s_send, s_recv, d_send, d_recv, p_send, p_recv, r_send, r_recv, loc,
):
    n_sp, n_tp, G, C, seqs, ppd, hl, block = dims
    n_o, J, JC = n_sp // G, G * n_tp, G * n_tp // C
    D = tok.shape[1]
    rows = wq.shape[0]
    kw = hl * KEY_DIM
    T = J * ppd
    nb = T // block
    i, t = lax.axis_index("sp"), lax.axis_index("tp")
    o, g = i // G, lax.rem(i, G)
    a, c = g // C, lax.rem(g, C)
    me_j = g * n_tp + t
    me_jj = a * n_tp + t
    partner = o * G + a * C + (1 - c)

    def remote(src, dst, send, recv, sp, tp):
        return pltpu.make_async_remote_copy(
            src_ref=src, dst_ref=dst, send_sem=send, recv_sem=recv, device_id=(sp, tp), device_id_type=MESH
        )

    def away():
        for da in range(G // C):
            for dt in range(n_tp):
                if da or dt:
                    yield da, dt

    def tok_copy(da, dt, sending):
        sign = 1 if sending else -1
        aa = lax.rem(a + sign * da + G // C, G // C)
        tt = lax.rem(t + sign * dt + n_tp, n_tp)
        gg = aa * C + c
        source = me_j if sending else gg * n_tp + tt
        return source, remote(
            tok, X.at[source], t_send.at[da * n_tp + dt], t_recv.at[source], o * G + gg, tt
        )

    for da, dt in away():
        tok_copy(da, dt, True)[1].start()
    own_tok = pltpu.make_async_copy(tok, X.at[me_j], loc.at[4])
    own_tok.start()
    if C > 1:
        to_partner = remote(tok, X.at[me_j], t_send.at[JC], t_recv.at[me_j], partner, t)
        to_partner.start()

    weights = (wf, wv, wq, wo)

    def w_copy(m, source, dest):
        cols = pl.ds(pl.multiple_of(lax.rem(dest, G) * kw, 128), kw)
        return remote(
            weights[m].at[:, cols],
            W.at[m, pl.ds(pl.multiple_of(source * rows, rows), rows), :],
            w_send.at[m, dest], w_recv.at[m, source], dest, t,
        )

    for m in range(4):
        def send_w(k, _, m=m):
            w_copy(m, i, lax.rem(i + k, n_sp)).start()
            return 0
        lax.fori_loop(1, n_sp, send_w, 0)
    own_cols = pl.ds(pl.multiple_of(g * kw, 128), kw)
    own_w = [
        pltpu.make_async_copy(
            weights[m].at[:, own_cols],
            W.at[m, pl.ds(pl.multiple_of(i * rows, rows), rows), :], loc.at[m],
        )
        for m in range(4)
    ]
    for copy in own_w:
        copy.start()

    def wait_w(m):
        def one(k, _):
            src = lax.rem(i + n_sp - k, n_sp)
            back = lax.rem(i, n_sp)
            cols = pl.ds(pl.multiple_of(lax.rem(back, G) * kw, 128), kw)
            remote(
                weights[m].at[:, cols],
                W.at[m, pl.ds(pl.multiple_of(src * rows, rows), rows), :],
                w_send.at[m, src], w_recv.at[m, src], src, t,
            ).wait_recv()
            return 0
        lax.fori_loop(1, n_sp, one, 0)
        own_w[m].wait()

    forwards = []
    for n, (da, dt) in enumerate(away()):
        source, copy = tok_copy(da, dt, False)
        copy.wait_recv()
        if C > 1:
            fwd = remote(X.at[source], X.at[source], t_send.at[JC + 1 + n], t_recv.at[source], partner, t)
            fwd.start()
            forwards.append(fwd)
    own_tok.wait()
    if C > 1:
        for da in range(G // C):
            for dt in range(n_tp):
                aa = lax.rem(a + da, G // C)
                tt = lax.rem(t + dt, n_tp)
                source = (aa * C + 1 - c) * n_tp + tt
                remote(tok, X.at[source], t_send.at[JC], t_recv.at[source], partner, t).wait_recv()

    step = math.gcd(seqs * ppd, 16)
    gain_row = gain[...]

    def norm_block(j, _):
        def norm_rows(r, _):
            where = pl.ds(pl.multiple_of(r * step, step), step)
            x = X[j, where, :].astype(f32)
            scale = lax.rsqrt(jnp.mean(x * x, axis=-1, keepdims=True) + eps_norm)
            N[j, where, :] = (x * scale * gain_row).astype(bf16)
            return 0
        lax.fori_loop(0, seqs * ppd // step, norm_rows, 0)
        return 0
    lax.fori_loop(0, J, norm_block, 0)

    per = max(1, min(J, 512 // (seqs * ppd)))

    def project(m):
        def tile(r, _):
            where = pl.ds(r * per, per)
            x = N[where].reshape(per * seqs * ppd, D)
            y = jnp.dot(x, W[m], preferred_element_type=f32).astype(bf16).astype(f32)
            PJ[m, where] = y.reshape(per, seqs, ppd, kw)
            return 0
        lax.fori_loop(0, J // per, tile, 0)

    wait_w(0)
    project(0)
    wait_w(1)
    project(1)

    gap_row = gap[:, own_cols]
    row_id = lax.broadcasted_iota(jnp.int32, (block, block), 0)
    col_id = lax.broadcasted_iota(jnp.int32, (block, block), 1)
    causal = row_id >= col_id
    ones = jnp.where(causal, 1.0, 0.0).astype(bf16)

    def head(h):
        return slice(h * KEY_DIM, (h + 1) * KEY_DIM)

    def state_copies(s, k, dest_o, src_o):
        sp = dest_o * G + g
        return (
            remote(SS.at[s], SR.at[src_o, s], s_send.at[k, s], s_recv.at[src_o, s], sp, t),
            remote(DS.at[s], DR.at[src_o, s], d_send.at[k, s], d_recv.at[src_o, s], sp, t),
        )

    def key_side(s, _):
        f = PJ[0, :, s].reshape(T, kw)
        v = PJ[1, :, s].reshape(T, kw).astype(bf16)
        inkey = gap_row * jax.nn.sigmoid(-f)
        log_forget = jnp.log1p(-inkey)
        IK[s] = inkey
        ends = [None] * hl
        total = None
        for b in range(nb):
            rs = slice(b * block, (b + 1) * block)
            lf = log_forget[rs]
            high = lf.astype(bf16)
            low = (lf - high.astype(f32)).astype(bf16)
            cum = jnp.dot(ones, high, preferred_element_type=f32) + jnp.dot(
                ones, low, preferred_element_type=f32
            )
            CUM[s, rs, :] = cum
            final = cum[block - 1 : block, :]
            dec = jnp.exp(final)
            DEC[s, b] = jnp.broadcast_to(dec, (8, kw))
            kf = (inkey[rs] * jnp.exp(final - cum)).astype(bf16)
            vb = v[rs]
            total = dec if total is None else total * dec
            for h in range(hl):
                u = tn(vb[:, head(h)], kf[:, head(h)])
                U[s, b, h] = u
                ends[h] = u if ends[h] is None else ends[h] * dec[:, head(h)] + u
        for h in range(hl):
            SS[s, h] = ends[h].astype(bf16)
        DS[s] = jnp.broadcast_to(total, (8, kw))

        def send(k, _):
            @pl.when(o + k < n_o)
            def _():
                for copy in state_copies(s, k, o + k, o):
                    copy.start()
            return 0
        lax.fori_loop(1, n_o, send, 0)
        return 0
    lax.fori_loop(0, seqs, key_side, 0)

    wait_w(2)
    project(2)

    def query_side(s, _):
        q = PJ[2, :, s].reshape(T, kw)
        v = PJ[1, :, s].reshape(T, kw).astype(bf16)
        q = q * jax.nn.sigmoid(q)
        for b in range(nb):
            rs = slice(b * block, (b + 1) * block)
            cum = CUM[s, rs, :]
            qs = (q[rs] * jnp.exp(cum)).astype(bf16)
            ks = (IK[s, rs, :] * jnp.exp(-cum)).astype(bf16)
            QS[s, rs, :] = qs
            vb = v[rs]
            for h in range(hl):
                scores = jnp.where(causal, nt(qs[:, head(h)], ks[:, head(h)]), 0.0).astype(bf16)
                INS[s, rs, head(h)] = jnp.dot(scores, vb[:, head(h)], preferred_element_type=f32)
        return 0
    lax.fori_loop(0, seqs, query_side, 0)

    wait_w(3)
    hg_row = hgain[:, own_cols]
    wide = math.gcd(D, 512)

    def pair_copy(s):
        return remote(OB.at[1 - c, :, s], PB.at[:, s], p_send.at[s], p_recv.at[s], partner, t)

    def plane_copy(da, dt, s, sending):
        sign = 1 if sending else -1
        aa = lax.rem(a + sign * da + G // C, G // C)
        tt = lax.rem(t + sign * dt + n_tp, n_tp)
        other = aa * n_tp + tt
        src, slot = (other, me_jj) if sending else (me_jj, other)
        return remote(
            RSB.at[src, s], RB.at[slot, s], r_send.at[da * n_tp + dt, s], r_recv.at[slot, s],
            o * G + aa * C + c, tt,
        )

    def finish(s):
        for h in range(hl):
            ACC[h] = jnp.zeros((VAL_DIM, KEY_DIM), f32)

        def earlier(k, _):
            @pl.when(k < o)
            def _():
                for copy in state_copies(s, 0, o, k):
                    copy.wait_recv()
                dec = DR[k, s][0:1, :]
                for h in range(hl):
                    ACC[h] = ACC[h] * dec[:, head(h)] + SR[k, s, h].astype(f32)
            return 0
        lax.fori_loop(0, n_o - 1, earlier, 0)
        for h in range(hl):
            state = ACC[h]
            for b in range(nb):
                rs = slice(b * block, (b + 1) * block)
                r = INS[s, rs, head(h)] + nt(QS[s, rs, head(h)], state.astype(bf16))
                scale = lax.rsqrt(jnp.mean(r * r, axis=-1, keepdims=True) + eps_norm)
                HB[rs, head(h)] = (r * scale * hg_row[:, head(h)]).astype(bf16)
                if b + 1 < nb:
                    state = state * DEC[s, b][0:1, head(h)] + U[s, b, h]
        hidden = HB[...]

        def columns(n, _):
            cs = pl.ds(pl.multiple_of(n * wide, wide), wide)
            y = nt(hidden, W[3, cs, :]).reshape(G // C, C, n_tp, ppd, wide)
            for par in range(C):
                OB[par, :, s, :, cs] = y[:, par].reshape(JC, ppd, wide).astype(bf16)
            return 0
        lax.fori_loop(0, D // wide, columns, 0)
        if C > 1:
            pair_copy(s).start()

    def reduce(s):
        if C > 1:
            pair_copy(s).wait_recv()

        def one(jj, _):
            if C > 1:
                RSB[jj, s] = (OB[c, jj, s].astype(f32) + PB[jj, s].astype(f32)).astype(bf16)
            else:
                RSB[jj, s] = OB[0, jj, s]
            return 0
        lax.fori_loop(0, JC, one, 0)
        for da, dt in away():
            plane_copy(da, dt, s, True).start()
        RB[me_jj, s] = RSB[me_jj, s]

    def pipeline(s, _):
        @pl.when(s < seqs)
        def _():
            finish(s)

        @pl.when(s > 0)
        def _():
            reduce(s - 1)
        return 0
    lax.fori_loop(0, seqs + 1, pipeline, 0)

    def last(s, _):
        for da, dt in away():
            plane_copy(da, dt, s, False).wait_recv()
        total = RB[0, s].astype(f32)
        for jj in range(1, JC):
            total = total + RB[jj, s].astype(f32)
        out[s] = total.astype(bf16)
        return 0
    lax.fori_loop(0, seqs, last, 0)

    for da, dt in away():
        tok_copy(da, dt, True)[1].wait_send()
    if C > 1:
        to_partner.wait_send()
        for fwd in forwards:
            fwd.wait_send()
    for m in range(4):
        def sent_w(k, _, m=m):
            w_copy(m, i, lax.rem(i + k, n_sp)).wait_send()
            return 0
        lax.fori_loop(1, n_sp, sent_w, 0)

    def sent(s, _):
        def states(k, _):
            @pl.when(o + k < n_o)
            def _():
                for copy in state_copies(s, k, o + k, o):
                    copy.wait_send()
            return 0
        lax.fori_loop(1, n_o, states, 0)
        if C > 1:
            pair_copy(s).wait_send()
        for da, dt in away():
            plane_copy(da, dt, s, True).wait_send()
        return 0
    lax.fori_loop(0, seqs, sent, 0)


def body(n_sp, n_tp, tokens, norm_gain, w_query, w_forget, w_value, floor_gap, head_gain, w_out):
    ppd, seqs, D = tokens.shape
    rows, width = w_query.shape
    heads = width // KEY_DIM
    G = math.gcd(math.gcd(n_sp, 4), max(1, heads // 2))
    C = 2 if G % 2 == 0 else 1
    hl = heads // G
    kw = hl * KEY_DIM
    n_o, J = n_sp // G, G * n_tp
    JC = J // C
    T = J * ppd
    block = math.gcd(T, 128)
    nb = T // block
    dims = (n_sp, n_tp, G, C, seqs, ppd, hl, block)
    vmem = pl.BlockSpec(memory_space=pltpu.VMEM)
    dma = pltpu.SemaphoreType.DMA
    result = pl.pallas_call(
        functools.partial(kernel, dims),
        out_shape=jax.ShapeDtypeStruct((seqs, ppd, D), bf16),
        in_specs=[vmem] * 8,
        out_specs=vmem,
        scratch_shapes=[
            pltpu.VMEM((J, seqs * ppd, D), bf16),
            pltpu.VMEM((J, seqs * ppd, D), bf16),
            pltpu.VMEM((4, n_sp * rows, kw), bf16),
            pltpu.VMEM((3, J, seqs, ppd, kw), f32),
            pltpu.VMEM((seqs, T, kw), f32),
            pltpu.VMEM((seqs, T, kw), f32),
            pltpu.VMEM((seqs, T, kw), bf16),
            pltpu.VMEM((seqs, T, kw), f32),
            pltpu.VMEM((seqs, nb, hl, VAL_DIM, KEY_DIM), f32),
            pltpu.VMEM((seqs, nb, 8, kw), f32),
            pltpu.VMEM((seqs, hl, VAL_DIM, KEY_DIM), bf16),
            pltpu.VMEM((seqs, 8, kw), f32),
            pltpu.VMEM((n_o, seqs, hl, VAL_DIM, KEY_DIM), bf16),
            pltpu.VMEM((n_o, seqs, 8, kw), f32),
            pltpu.VMEM((hl, VAL_DIM, KEY_DIM), f32),
            pltpu.VMEM((T, kw), bf16),
            pltpu.VMEM((C, JC, seqs, ppd, D), bf16),
            pltpu.VMEM((JC, seqs, ppd, D), bf16),
            pltpu.VMEM((JC, seqs, ppd, D), bf16),
            pltpu.VMEM((JC, seqs, ppd, D), bf16),
            dma((4, n_sp)), dma((4, n_sp)),
            dma((2 * JC + 1,)), dma((J,)),
            dma((n_o, seqs)), dma((n_o, seqs)),
            dma((n_o, seqs)), dma((n_o, seqs)),
            dma((seqs,)), dma((seqs,)),
            dma((JC, seqs)), dma((JC, seqs)),
            dma((5,)),
        ],
        compiler_params=pltpu.CompilerParams(has_side_effects=True, vmem_limit_bytes=62 * 1024 * 1024),
        name="block",
    )(
        tokens.transpose(1, 0, 2).reshape(seqs * ppd, D),
        norm_gain.reshape(1, D), w_query, w_forget, w_value, w_out.T,
        floor_gap.reshape(1, width), head_gain.reshape(1, width),
    )
    return result.transpose(1, 0, 2)


def solution(mesh):
    return jax.shard_map(
        functools.partial(body, mesh.shape["sp"], mesh.shape["tp"]),
        mesh=mesh,
        in_specs=(
            P(("sp", "tp"), None, None),
            P(),
            P("sp", "tp"),
            P("sp", "tp"),
            P("sp", "tp"),
            P("tp"),
            P("tp"),
            P("tp", "sp"),
        ),
        out_specs=P(("sp", "tp"), None, None),
        check_vma=False,
    )
```

```python
import functools
import math

import jax
import jax.numpy as jnp
from jax import lax
from jax.experimental import pallas as pl
from jax.experimental.pallas import tpu as pltpu
from jax.sharding import PartitionSpec as P

KEY_DIM = 128
VAL_DIM = 128
eps_norm = 1e-06
MESH = pl.DeviceIdType.MESH
f32 = jnp.float32
bf16 = jnp.bfloat16


def nt(a, b):
    return lax.dot_general(a, b, (((1,), (1,)), ((), ())), preferred_element_type=f32)


def tn(a, b):
    return lax.dot_general(a, b, (((0,), (0,)), ((), ())), preferred_element_type=f32)


def kernel(
    dims,
    tok, gain, wq, wf, wv, wo, gap, hgain,
    out,
    X, N, W, PJ, IK, CUM, QS, INS, U, DEC, EL, DT, SS, SR, ACC, HB, OB, PB, RSB, RB,
    w_send, w_recv, z_send, z_recv, t_send, t_recv, s_send, s_recv, p_send, p_recv, r_send, r_recv, loc,
):
    n_sp, n_tp, G, C, seqs, ppd, hl, block = dims
    n_o, J, JC = n_sp // G, G * n_tp, G * n_tp // C
    D = tok.shape[1]
    rows = wq.shape[0]
    kw = hl * KEY_DIM
    T = J * ppd
    nb = T // block
    i, t = lax.axis_index("sp"), lax.axis_index("tp")
    o, g = i // G, lax.rem(i, G)
    a, c = g // C, lax.rem(g, C)
    me_j = g * n_tp + t
    me_jj = a * n_tp + t
    partner = o * G + a * C + (1 - c)

    def remote(src, dst, send, recv, sp, tp):
        return pltpu.make_async_remote_copy(
            src_ref=src, dst_ref=dst, send_sem=send, recv_sem=recv, device_id=(sp, tp), device_id_type=MESH
        )

    def away():
        for da in range(G // C):
            for dt in range(n_tp):
                if da or dt:
                    yield da, dt

    def tok_copy(da, dt, sending):
        sign = 1 if sending else -1
        aa = lax.rem(a + sign * da + G // C, G // C)
        tt = lax.rem(t + sign * dt + n_tp, n_tp)
        gg = aa * C + c
        source = me_j if sending else gg * n_tp + tt
        return source, remote(
            tok, X.at[source], t_send.at[da * n_tp + dt], t_recv.at[source], o * G + gg, tt
        )

    weights = (wf, wv, wq, wo)
    n_w = len(weights)

    def block_of(m, b):
        return W.at[m, pl.ds(pl.multiple_of(b * G * rows, G * rows), G * rows), :]

    def slice_of(m, source):
        return W.at[m, pl.ds(pl.multiple_of(source * rows, rows), rows), :]

    def plane_w(m, k):
        gg = lax.rem(g + k, G)
        cols = pl.ds(pl.multiple_of(gg * kw, 128), kw)
        return remote(
            weights[m].at[:, cols], slice_of(m, i), w_send.at[m, k], w_recv.at[m, k], o * G + gg, t
        )

    def line_w(m, b, way):
        return remote(
            block_of(m, b), block_of(m, b), z_send.at[way, m, b], z_recv.at[m, b],
            (o + 1 - 2 * way) * G + g, t,
        )

    own_cols = pl.ds(pl.multiple_of(g * kw, 128), kw)
    for m in range(n_w):
        for k in range(1, G):
            plane_w(m, k).start()
        pltpu.make_async_copy(weights[m].at[:, own_cols], slice_of(m, i), loc.at[m]).start()

    for da, dt in away():
        tok_copy(da, dt, True)[1].start()
    own_tok = pltpu.make_async_copy(tok, X.at[me_j], loc.at[n_w])
    own_tok.start()
    if C > 1:
        to_partner = remote(tok, X.at[me_j], t_send.at[JC], t_recv.at[me_j], partner, t)
        to_partner.start()

    def stage(d):
        def first(m):
            for k in range(1, G):
                gg = lax.rem(g - k + G, G)
                here = slice_of(m, o * G + gg)
                remote(here, here, w_send.at[m, k], w_recv.at[m, k], o * G + gg, t).wait_recv()
            pltpu.make_async_copy(slice_of(m, i), slice_of(m, i), loc.at[m]).wait()

            @pl.when(o + 1 < n_o)
            def _():
                line_w(m, o, 0).start()

            @pl.when(o > 0)
            def _():
                line_w(m, o, 1).start()

        def hop(r, _):
            m = d - r

            @pl.when((m >= 0) & (m < n_w) & (o - r >= 0))
            def _():
                line_w(m, o - r, 1).wait_recv()

                @pl.when(o + 1 < n_o)
                def _():
                    line_w(m, o - r, 0).start()

            @pl.when((m >= 0) & (m < n_w) & (o + r < n_o))
            def _():
                line_w(m, o + r, 0).wait_recv()

                @pl.when(o > 0)
                def _():
                    line_w(m, o + r, 1).start()
            return 0

        if isinstance(d, int):
            if d < n_w:
                first(d)
        else:
            @pl.when(d < n_w)
            def _():
                first(d)
        lax.fori_loop(1, n_o, hop, 0)

    def early(d, _):
        stage(d)
        return 0
    lax.fori_loop(0, n_o - 1, early, 0)
    stage(n_o - 1)

    forwards = []
    for n, (da, dt) in enumerate(away()):
        source, copy = tok_copy(da, dt, False)
        copy.wait_recv()
        if C > 1:
            fwd = remote(X.at[source], X.at[source], t_send.at[JC + 1 + n], t_recv.at[source], partner, t)
            fwd.start()
            forwards.append(fwd)
    own_tok.wait()
    if C > 1:
        for da in range(G // C):
            for dt in range(n_tp):
                aa = lax.rem(a + da, G // C)
                tt = lax.rem(t + dt, n_tp)
                source = (aa * C + 1 - c) * n_tp + tt
                remote(tok, X.at[source], t_send.at[JC], t_recv.at[source], partner, t).wait_recv()

    step = math.gcd(seqs * ppd, 16)
    gain_row = gain[...]

    def norm_block(j, _):
        def norm_rows(r, _):
            where = pl.ds(pl.multiple_of(r * step, step), step)
            x = X[j, where, :].astype(f32)
            scale = lax.rsqrt(jnp.mean(x * x, axis=-1, keepdims=True) + eps_norm)
            N[j, where, :] = (x * scale * gain_row).astype(bf16)
            return 0
        lax.fori_loop(0, seqs * ppd // step, norm_rows, 0)
        return 0
    lax.fori_loop(0, J, norm_block, 0)

    per = max(1, min(J, 512 // (seqs * ppd)))

    def project(m):
        def tile(r, _):
            where = pl.ds(r * per, per)
            x = N[where].reshape(per * seqs * ppd, D)
            y = jnp.dot(x, W[m], preferred_element_type=f32).astype(bf16).astype(f32)
            PJ[m, where] = y.reshape(per, seqs, ppd, kw)
            return 0
        lax.fori_loop(0, J // per, tile, 0)

    project(0)
    stage(n_o)
    project(1)

    gap_row = gap[:, own_cols]
    row_id = lax.broadcasted_iota(jnp.int32, (block, block), 0)
    col_id = lax.broadcasted_iota(jnp.int32, (block, block), 1)
    causal = row_id >= col_id
    ones = jnp.where(causal, 1.0, 0.0).astype(bf16)

    def head(h):
        return slice(h * KEY_DIM, (h + 1) * KEY_DIM)

    def chain_copy(s):
        return remote(SS.at[s], SR.at[s], s_send.at[s], s_recv.at[s], (o + 1) * G + g, t)

    def chain(s):
        @pl.when(o > 0)
        def _():
            chain_copy(s).wait_recv()

            @pl.when(o + 1 < n_o)
            def _():
                for h in range(hl):
                    incoming = SR[s, h].astype(f32)
                    SS[s, h] = (incoming * DT[s][0:1, head(h)] + EL[s, h]).astype(bf16)
                chain_copy(s).start()

    def key_side(s, _):
        f = PJ[0, :, s].reshape(T, kw)
        v = PJ[1, :, s].reshape(T, kw).astype(bf16)
        inkey = gap_row * jax.nn.sigmoid(-f)
        log_forget = jnp.log1p(-inkey)
        IK[s] = inkey
        ends = [None] * hl
        total = None
        for b in range(nb):
            rs = slice(b * block, (b + 1) * block)
            lf = log_forget[rs]
            high = lf.astype(bf16)
            low = (lf - high.astype(f32)).astype(bf16)
            cum = jnp.dot(ones, high, preferred_element_type=f32) + jnp.dot(
                ones, low, preferred_element_type=f32
            )
            CUM[s, rs, :] = cum
            final = cum[block - 1 : block, :]
            dec = jnp.exp(final)
            DEC[s, b] = jnp.broadcast_to(dec, (8, kw))
            kf = (inkey[rs] * jnp.exp(final - cum)).astype(bf16)
            vb = v[rs]
            total = dec if total is None else total * dec
            for h in range(hl):
                u = tn(vb[:, head(h)], kf[:, head(h)])
                U[s, b, h] = u
                ends[h] = u if ends[h] is None else ends[h] * dec[:, head(h)] + u
        for h in range(hl):
            EL[s, h] = ends[h]
        DT[s] = jnp.broadcast_to(total, (8, kw))

        @pl.when((o == 0) & (n_o > 1))
        def _():
            for h in range(hl):
                SS[s, h] = ends[h].astype(bf16)
            chain_copy(s).start()
        return 0
    lax.fori_loop(0, seqs, key_side, 0)

    stage(n_o + 1)
    project(2)

    def query_side(s, _):
        q = PJ[2, :, s].reshape(T, kw)
        v = PJ[1, :, s].reshape(T, kw).astype(bf16)
        q = q * jax.nn.sigmoid(q)
        for b in range(nb):
            rs = slice(b * block, (b + 1) * block)
            cum = CUM[s, rs, :]
            qs = (q[rs] * jnp.exp(cum)).astype(bf16)
            ks = (IK[s, rs, :] * jnp.exp(-cum)).astype(bf16)
            QS[s, rs, :] = qs
            vb = v[rs]
            for h in range(hl):
                scores = jnp.where(causal, nt(qs[:, head(h)], ks[:, head(h)]), 0.0).astype(bf16)
                INS[s, rs, head(h)] = jnp.dot(scores, vb[:, head(h)], preferred_element_type=f32)
        chain(s)
        return 0
    lax.fori_loop(0, seqs, query_side, 0)

    stage(n_o + 2)
    hg_row = hgain[:, own_cols]
    wide = math.gcd(D, 512)

    def pair_copy(s):
        return remote(OB.at[1 - c, :, s], PB.at[:, s], p_send.at[s], p_recv.at[s], partner, t)

    def plane_copy(da, dt, s, sending):
        sign = 1 if sending else -1
        aa = lax.rem(a + sign * da + G // C, G // C)
        tt = lax.rem(t + sign * dt + n_tp, n_tp)
        other = aa * n_tp + tt
        src, slot = (other, me_jj) if sending else (me_jj, other)
        return remote(
            RSB.at[src, s], RB.at[slot, s], r_send.at[da * n_tp + dt, s], r_recv.at[slot, s],
            o * G + aa * C + c, tt,
        )

    def finish(s):
        ACC[...] = jnp.zeros_like(ACC)

        @pl.when(o > 0)
        def _():
            ACC[...] = SR[s].astype(f32)

        for h in range(hl):
            state = ACC[h]
            for b in range(nb):
                rs = slice(b * block, (b + 1) * block)
                r = INS[s, rs, head(h)] + nt(QS[s, rs, head(h)], state.astype(bf16))
                scale = lax.rsqrt(jnp.mean(r * r, axis=-1, keepdims=True) + eps_norm)
                HB[rs, head(h)] = (r * scale * hg_row[:, head(h)]).astype(bf16)
                if b + 1 < nb:
                    state = state * DEC[s, b][0:1, head(h)] + U[s, b, h]
        hidden = HB[...]

        def columns(n, _):
            cs = pl.ds(pl.multiple_of(n * wide, wide), wide)
            y = nt(hidden, W[3, cs, :]).reshape(G // C, C, n_tp, ppd, wide)
            for par in range(C):
                OB[par, :, s, :, cs] = y[:, par].reshape(JC, ppd, wide).astype(bf16)
            return 0
        lax.fori_loop(0, D // wide, columns, 0)
        if C > 1:
            pair_copy(s).start()

    def reduce(s):
        if C > 1:
            pair_copy(s).wait_recv()

        def one(jj, _):
            if C > 1:
                RSB[jj, s] = (OB[c, jj, s].astype(f32) + PB[jj, s].astype(f32)).astype(bf16)
            else:
                RSB[jj, s] = OB[0, jj, s]
            return 0
        lax.fori_loop(0, JC, one, 0)
        for da, dt in away():
            plane_copy(da, dt, s, True).start()
        RB[me_jj, s] = RSB[me_jj, s]

    def pipeline(s, _):
        @pl.when(s < seqs)
        def _():
            finish(s)

        @pl.when(s > 0)
        def _():
            reduce(s - 1)
        return 0
    lax.fori_loop(0, seqs + 1, pipeline, 0)

    def last(s, _):
        for da, dt in away():
            plane_copy(da, dt, s, False).wait_recv()
        total = RB[0, s].astype(f32)
        for jj in range(1, JC):
            total = total + RB[jj, s].astype(f32)
        out[s] = total.astype(bf16)
        return 0
    lax.fori_loop(0, seqs, last, 0)

    for da, dt in away():
        tok_copy(da, dt, True)[1].wait_send()
    if C > 1:
        to_partner.wait_send()
        for fwd in forwards:
            fwd.wait_send()
    for m in range(n_w):
        for k in range(1, G):
            plane_w(m, k).wait_send()

        def sent_w(b, _, m=m):
            @pl.when((b <= o) & (o + 1 < n_o))
            def _():
                line_w(m, b, 0).wait_send()

            @pl.when((b >= o) & (o > 0))
            def _():
                line_w(m, b, 1).wait_send()
            return 0
        lax.fori_loop(0, n_o, sent_w, 0)

    def sent(s, _):
        @pl.when(o + 1 < n_o)
        def _():
            chain_copy(s).wait_send()
        if C > 1:
            pair_copy(s).wait_send()
        for da, dt in away():
            plane_copy(da, dt, s, True).wait_send()
        return 0
    lax.fori_loop(0, seqs, sent, 0)


def body(n_sp, n_tp, tokens, norm_gain, w_query, w_forget, w_value, floor_gap, head_gain, w_out):
    ppd, seqs, D = tokens.shape
    rows, width = w_query.shape
    heads = width // KEY_DIM
    G = math.gcd(math.gcd(n_sp, 4), max(1, heads // 2))
    C = 2 if G % 2 == 0 else 1
    hl = heads // G
    kw = hl * KEY_DIM
    n_o, J = n_sp // G, G * n_tp
    JC = J // C
    T = J * ppd
    block = math.gcd(T, 128)
    nb = T // block
    dims = (n_sp, n_tp, G, C, seqs, ppd, hl, block)
    vmem = pl.BlockSpec(memory_space=pltpu.VMEM)
    dma = pltpu.SemaphoreType.DMA
    result = pl.pallas_call(
        functools.partial(kernel, dims),
        out_shape=jax.ShapeDtypeStruct((seqs, ppd, D), bf16),
        in_specs=[vmem] * 8,
        out_specs=vmem,
        scratch_shapes=[
            pltpu.VMEM((J, seqs * ppd, D), bf16),
            pltpu.VMEM((J, seqs * ppd, D), bf16),
            pltpu.VMEM((4, n_sp * rows, kw), bf16),
            pltpu.VMEM((3, J, seqs, ppd, kw), f32),
            pltpu.VMEM((seqs, T, kw), f32),
            pltpu.VMEM((seqs, T, kw), f32),
            pltpu.VMEM((seqs, T, kw), bf16),
            pltpu.VMEM((seqs, T, kw), f32),
            pltpu.VMEM((seqs, nb, hl, VAL_DIM, KEY_DIM), f32),
            pltpu.VMEM((seqs, nb, 8, kw), f32),
            pltpu.VMEM((seqs, hl, VAL_DIM, KEY_DIM), f32),
            pltpu.VMEM((seqs, 8, kw), f32),
            pltpu.VMEM((seqs, hl, VAL_DIM, KEY_DIM), bf16),
            pltpu.VMEM((seqs, hl, VAL_DIM, KEY_DIM), bf16),
            pltpu.VMEM((hl, VAL_DIM, KEY_DIM), f32),
            pltpu.VMEM((T, kw), bf16),
            pltpu.VMEM((C, JC, seqs, ppd, D), bf16),
            pltpu.VMEM((JC, seqs, ppd, D), bf16),
            pltpu.VMEM((JC, seqs, ppd, D), bf16),
            pltpu.VMEM((JC, seqs, ppd, D), bf16),
            dma((4, G)), dma((4, G)),
            dma((2, 4, n_o)), dma((4, n_o)),
            dma((2 * JC + 1,)), dma((J,)),
            dma((seqs,)), dma((seqs,)),
            dma((seqs,)), dma((seqs,)),
            dma((JC, seqs)), dma((JC, seqs)),
            dma((5,)),
        ],
        compiler_params=pltpu.CompilerParams(has_side_effects=True, vmem_limit_bytes=62 * 1024 * 1024),
        name="block",
    )(
        tokens.transpose(1, 0, 2).reshape(seqs * ppd, D),
        norm_gain.reshape(1, D), w_query, w_forget, w_value, w_out.T,
        floor_gap.reshape(1, width), head_gain.reshape(1, width),
    )
    return result.transpose(1, 0, 2)


def solution(mesh):
    return jax.shard_map(
        functools.partial(body, mesh.shape["sp"], mesh.shape["tp"]),
        mesh=mesh,
        in_specs=(
            P(("sp", "tp"), None, None),
            P(),
            P("sp", "tp"),
            P("sp", "tp"),
            P("sp", "tp"),
            P("tp"),
            P("tp"),
            P("tp", "sp"),
        ),
        out_specs=P(("sp", "tp"), None, None),
        check_vma=False,
    )
```
